32 devices in a mesh: kv: 8 (over z, y), tp: 4 (over x, core).
Axes of the slice: x: 2, y: 2, z: 4, core: 2. Of those that a mesh axis runs over, the one named last changes fastest.
Arguments:
- tokens: bfloat16 [256, 4096], P(None, ('kv', 'tp')), may hold values from -60 to 60
- past_state: float32 [256, 16, 128, 128], P('kv', 'tp'), may hold values from -4 to 4
- pre_gain: float32 [4096], replicated, may hold values from 0.1 to 1.9
- pre_gate: bfloat16 [4096, 11264], P(None, ('kv', 'tp')), may hold values from -0.09375 to 0.09375
- pre_up: bfloat16 [4096, 11264], P(None, ('kv', 'tp')), may hold values from -0.09375 to 0.09375
- pre_down: bfloat16 [11264, 4096], P(('kv', 'tp')), may hold values from -0.109375 to 0.109375
- mix_gain: float32 [4096], replicated, may hold values from 0.1 to 1.9
- query_weight: bfloat16 [4096, 2048], P('kv', 'tp'), may hold values from -0.09375 to 0.09375
- forget_weight: bfloat16 [4096, 2048], P('kv', 'tp'), may hold values from -0.09375 to 0.09375
- value_weight: bfloat16 [4096, 2048], P('kv', 'tp'), may hold values from -0.09375 to 0.09375
- output_gate_weight: bfloat16 [4096, 2048], P('kv', 'tp'), may hold values from -0.09375 to 0.09375
- forget_floor: float32 [2048], P('tp'), may hold values from 0.02 to 0.9
- head_gain: float32 [128], replicated, may hold values from 0.1 to 1.9
- proj_out: bfloat16 [2048, 4096], P('tp', 'kv'), may hold values from -0.125 to 0.125
- post_gain: float32 [4096], replicated, may hold values from 0.1 to 1.9
- post_gate: bfloat16 [4096, 11264], P(None, ('kv', 'tp')), may hold values from -0.09375 to 0.09375
- post_up: bfloat16 [4096, 11264], P(None, ('kv', 'tp')), may hold values from -0.09375 to 0.09375
- post_down: bfloat16 [11264, 4096], P(('kv', 'tp')), may hold values from -0.109375 to 0.109375
Outputs:
- result: bfloat16 [256, 4096], P(None, ('kv', 'tp'))
- new_state: float32 [256, 16, 128, 128], P('kv', 'tp')
The draws below stay inside these ranges and needn't reach their ends.
All inputs are finite; a program needn't handle non-finite values.
Results may differ from the reference program's by a relative error of at most 0.014.
Values may be sent and summed in bfloat16 or wider, within the bound.
A program may use at most 128 MiB of HBM per device.

```python
import math
import jax
import jax.numpy as jnp
from jax import lax

D = 4096
FF = 11264
HEADS = 16
HEAD_DIM = 128
INNER = 2048
SEQS = 256
N_TP = 4


def draw_tokens(key, part):
    key_base = jax.random.fold_in(key, 11)
    key_rows = jax.random.fold_in(key, 12)
    key_cols = jax.random.fold_in(key, 13)
    column_pos = jnp.arange(D, dtype=jnp.float32) / D
    jitter = jax.random.uniform(key_cols, (1, D), jnp.float32, 0.7, 1.3)
    rising = 0.5 * jnp.exp(column_pos * jnp.log(4.0))
    row_scales = jnp.exp(jax.random.uniform(key_rows, (SEQS, 1), jnp.float32, jnp.log(0.5), jnp.log(5.0)))
    base_vals = jnp.clip(jax.random.normal(key_base, (SEQS, D), jnp.float32), -4.0, 4.0)
    return (base_vals * rising[None, :] * jitter * row_scales).astype(jnp.bfloat16)


def spiked(values, stream_key, source, target, parts, factor):
    def block_of(dim):
        return (jnp.arange(values.shape[dim]) // (values.shape[dim] // parts)).reshape((-1,) + (1,) * (values.ndim - 1 - dim))

    near = jax.random.permutation(stream_key, parts)[block_of(target)]
    second = (block_of(target) + parts // 2) % parts
    return jnp.where((block_of(source) == near) | (block_of(source) == second), factor * values, values)


def shard_levels(stream_key, dims, cuts, smallest, high):
    level, own = 1.0, jax.random.fold_in(stream_key, 6)
    for position, parts in cuts:
        steps = jnp.exp(jax.random.uniform(jax.random.fold_in(own, position), (parts,), jnp.float32, smallest / len(cuts), high / len(cuts)))
        level = level * jnp.repeat(steps, dims[position] // parts).reshape([-1 if axis == position else 1 for axis in range(len(dims))])
    return level


def scatter_about(rng, dims, scale, bound, split=(), kind=jnp.bfloat16):
    level = shard_levels(rng, dims, split, -0.22, 0.18) if split else 1.0
    values = jax.random.normal(rng, dims, jnp.float32) * scale * level
    return jnp.minimum(jnp.maximum(values, -bound), bound).astype(kind)


def bell_draw_with(own_key, extent, deviation, limit, cuts, heavy, kind=jnp.bfloat16):
    entries = deviation * jax.random.normal(own_key, extent, jnp.float32)
    if cuts:
        entries = entries * shard_levels(own_key, extent, cuts, -0.22, 0.18)
    return jnp.clip(spiked(entries, jax.random.fold_in(own_key, 3), *heavy), -limit, limit).astype(kind)


def setup_inputs(seed: int = 0) -> dict:
    keys = jax.random.split(jax.random.key(seed), 19)
    return {
        "tokens": draw_tokens(jax.random.fold_in(keys[18], 71), 0),
        "past_state": scatter_about(keys[1], (SEQS, HEADS, HEAD_DIM, HEAD_DIM), 0.3, 4.0, ((0, 8), (1, 4)), jnp.float32),
        "pre_gain": jnp.clip(1.0 + 0.18 * jax.random.normal(keys[2], (D,), jnp.float32), 0.1, 1.9),
        "pre_gate": scatter_about(keys[3], (D, FF), D ** -0.5, 0.09375, ((1, 32),)),
        "pre_up": scatter_about(keys[4], (D, FF), D ** -0.5, 0.09375, ((1, 32),)),
        "pre_down": bell_draw_with(keys[5], (FF, D), FF ** -0.5, 0.109375, ((0, 32),), (0, 1, 32, 2.75)),
        "mix_gain": jnp.clip(1.0 + 0.18 * jax.random.normal(keys[6], (D,), jnp.float32), 0.1, 1.9),
        "query_weight": scatter_about(keys[7], (D, INNER), D ** -0.5, 0.09375, ((0, 8), (1, 4))),
        "forget_weight": scatter_about(keys[8], (D, INNER), D ** -0.5, 0.09375, ((0, 8), (1, 4))),
        "value_weight": scatter_about(keys[9], (D, INNER), D ** -0.5, 0.09375, ((0, 8), (1, 4))),
        "output_gate_weight": scatter_about(keys[10], (D, INNER), D ** -0.5, 0.09375, ((0, 8), (1, 4))),
        "forget_floor": jnp.clip(jnp.exp(math.log(0.9) - 3.8066625 * jax.random.uniform(keys[11], (INNER,), jnp.float32) ** shard_levels(keys[11], (INNER,), ((0, 4),), -0.2, 0.2)), 0.02, 0.9),
        "head_gain": jnp.clip(1.0 + 0.18 * jax.random.normal(keys[12], (HEAD_DIM,), jnp.float32), 0.1, 1.9),
        "proj_out": scatter_about(keys[13], (INNER, D), INNER ** -0.5, 0.125, ((0, 4), (1, 8))),
        "post_gain": jnp.clip(1.0 + 0.18 * jax.random.normal(keys[14], (D,), jnp.float32), 0.1, 1.9),
        "post_gate": scatter_about(keys[15], (D, FF), D ** -0.5, 0.09375, ((1, 32),)),
        "post_up": scatter_about(keys[16], (D, FF), D ** -0.5, 0.09375, ((1, 32),)),
        "post_down": bell_draw_with(keys[17], (FF, D), FF ** -0.5, 0.109375, ((0, 32),), (0, 1, 32, 2.75)),
    }


epsilon = 1e-06

def half_step(activations, gain, w_gate, w_up, w_down):
    x_float = activations.astype(jnp.float32)
    row_scale = lax.rsqrt(lax.optimization_barrier(jnp.mean(x_float * x_float, axis=1, keepdims=True)) + epsilon)
    normed = (x_float * gain).astype(jnp.bfloat16)
    gate_pre = row_scale * jnp.dot(normed, w_gate, preferred_element_type=jnp.float32)
    up_pre = row_scale * jnp.dot(normed, w_up, preferred_element_type=jnp.float32)
    hidden = (jax.nn.silu(gate_pre) * up_pre).astype(jnp.bfloat16)
    down_out = jnp.dot(hidden, w_down, preferred_element_type=jnp.float32)
    return (x_float + 0.5 * down_out).astype(jnp.bfloat16)

def reference(tokens, past_state, pre_gain, pre_gate, pre_up, pre_down, mix_gain, query_weight, forget_weight, value_weight, output_gate_weight, forget_floor, head_gain, proj_out, post_gain, post_gate, post_up, post_down):
    after_first = half_step(tokens, pre_gain, pre_gate, pre_up, pre_down)
    first_float = after_first.astype(jnp.float32)
    row_scale = lax.rsqrt(lax.optimization_barrier(jnp.mean(first_float * first_float, axis=1, keepdims=True)) + epsilon)
    normed = (first_float * mix_gain).astype(jnp.bfloat16)
    row_count = tokens.shape[0]
    head_shape = (row_count, HEADS, HEAD_DIM)
    pre_query = row_scale * jnp.dot(normed, query_weight, preferred_element_type=jnp.float32)
    pre_forget = row_scale * jnp.dot(normed, forget_weight, preferred_element_type=jnp.float32)
    pre_value = row_scale * jnp.dot(normed, value_weight, preferred_element_type=jnp.float32)
    pre_gate_out = row_scale * jnp.dot(normed, output_gate_weight, preferred_element_type=jnp.float32)
    floors = forget_floor.reshape(HEADS, HEAD_DIM)
    forget_heads = pre_forget.reshape(head_shape)
    forget = floors + (1.0 - floors) * jax.nn.sigmoid(forget_heads)
    written = (1.0 - floors) * jax.nn.sigmoid(-forget_heads)
    query_act = jax.nn.silu(pre_query.reshape(head_shape))
    value_act = pre_value.reshape(head_shape)
    new_state = forget[:, :, :, None] * past_state + written[:, :, :, None] * value_act[:, :, None, :]
    readout = jnp.einsum('bhkv,bhk->bhv', new_state, query_act, precision=lax.Precision.HIGHEST)
    readout = readout * lax.rsqrt(lax.optimization_barrier(jnp.mean(readout * readout, axis=2, keepdims=True)) + epsilon) * head_gain
    mixed_in = (readout.reshape(row_count, INNER) * jax.nn.silu(pre_gate_out)).astype(jnp.bfloat16)
    per_group = INNER // N_TP
    total_sum = jnp.zeros((row_count, D), jnp.float32)
    for head_block in range(N_TP):
        lower = head_block * per_group
        partial_out = jnp.dot(mixed_in[:, lower:lower + per_group], proj_out[lower:lower + per_group], preferred_element_type=jnp.float32).astype(jnp.bfloat16)
        total_sum = total_sum + partial_out.astype(jnp.float32)
    second = (first_float + total_sum).astype(jnp.bfloat16)
    result = half_step(second, post_gain, post_gate, post_up, post_down)
    return (result, new_state)
```

```python
import functools

import jax
import jax.numpy as jnp
from jax import lax
from jax.experimental import pallas as pl
from jax.experimental.pallas import tpu as pltpu
from jax.sharding import PartitionSpec as P

D = 4096


epsilon = 1e-06


def half_inputs(activations, gain, w_gate, w_up):
    piece_float = lax.all_gather(activations, ("kv", "tp"), axis=1, tiled=True).astype(jnp.float32)
    normed = (piece_float * gain).astype(jnp.bfloat16)
    gate_acc = jnp.dot(normed, w_gate, preferred_element_type=jnp.float32)
    up_acc = jnp.dot(normed, w_up, preferred_element_type=jnp.float32)
    squares = jnp.sum(piece_float * piece_float, axis=1)
    row_scale = lax.rsqrt(squares / D + epsilon)[:, None]
    return (jax.nn.silu(row_scale * gate_acc) * (row_scale * up_acc)).astype(jnp.bfloat16)


def down_sum(hidden, w_down):
    return lax.psum_scatter(
        jnp.dot(hidden, w_down, preferred_element_type=jnp.float32),
        ("kv", "tp"),
        scatter_dimension=1,
        tiled=True,
    )


def per_device_plain(
    tokens,
    past_state,
    pre_gain,
    pre_gate,
    pre_up,
    pre_down,
    mix_gain,
    query_weight,
    forget_weight,
    value_weight,
    output_gate_weight,
    forget_floor,
    head_gain,
    proj_out,
    post_gain,
    post_gate,
    post_up,
    post_down,
):
    whole_rows = lax.all_gather(tokens, ("kv", "tp"), axis=1, tiled=True)
    whole_float = whole_rows.astype(jnp.float32)
    row_scale = lax.rsqrt(jnp.mean(whole_float * whole_float, axis=1, keepdims=True) + epsilon)
    normed = (whole_float * pre_gain).astype(jnp.bfloat16)
    gate_pre = row_scale * jnp.dot(normed, pre_gate, preferred_element_type=jnp.float32)
    up_pre = row_scale * jnp.dot(normed, pre_up, preferred_element_type=jnp.float32)
    hidden = (jax.nn.silu(gate_pre) * up_pre).astype(jnp.bfloat16)
    kv_sums = lax.psum_scatter(
        jnp.dot(hidden, pre_down, preferred_element_type=jnp.float32).astype(jnp.bfloat16),
        "kv",
        scatter_dimension=1,
        tiled=True,
    )
    block_sum = lax.psum(kv_sums, "tp").astype(jnp.float32)
    block_width = block_sum.shape[1]
    block_old = lax.dynamic_slice_in_dim(
        whole_rows, lax.axis_index("kv") * block_width, block_width, 1
    )
    block_rows = (block_old.astype(jnp.float32) + 0.5 * block_sum).astype(jnp.bfloat16)
    own_width = block_width // lax.axis_size("tp")
    after_first = lax.dynamic_slice_in_dim(
        block_rows, lax.axis_index("tp") * own_width, own_width, 1
    )
    block_width = block_rows.shape[1]
    block_float = block_rows.astype(jnp.float32)
    block_gain = lax.dynamic_slice_in_dim(
        mix_gain, lax.axis_index("kv") * block_width, block_width, 0
    )
    squares = lax.psum(jnp.sum(block_float * block_float, axis=1), "kv")
    normed = (block_float * block_gain).astype(jnp.bfloat16)
    own_rows = past_state.shape[0]
    weight_list = (query_weight, forget_weight, value_weight, output_gate_weight)
    projected = lax.psum_scatter(
        jnp.concatenate(
            [
                jnp.dot(normed, weight_part, preferred_element_type=jnp.float32)
                for weight_part in weight_list
            ],
            axis=1,
        ).astype(jnp.bfloat16),
        "kv",
        scatter_dimension=0,
        tiled=True,
    ).astype(jnp.float32)
    own_squares = lax.dynamic_slice_in_dim(squares, lax.axis_index("kv") * own_rows, own_rows, 0)
    projected = projected * lax.rsqrt(own_squares / D + epsilon)[:, None]
    pre_query, pre_forget, pre_value, pre_gate_out = jnp.split(projected, 4, axis=1)
    local_heads = past_state.shape[1]
    head_width = past_state.shape[2]
    head_shape = (own_rows, local_heads, head_width)
    floors = forget_floor.reshape(local_heads, head_width)
    forget_heads = pre_forget.reshape(head_shape)
    forget = floors + (1.0 - floors) * jax.nn.sigmoid(forget_heads)
    written = (1.0 - floors) * jax.nn.sigmoid(-forget_heads)
    query_act = jax.nn.silu(pre_query.reshape(head_shape))
    value_act = pre_value.reshape(head_shape)
    new_state = (
        forget[:, :, :, None] * past_state + written[:, :, :, None] * value_act[:, :, None, :]
    )
    readout = jnp.einsum("bhkv,bhk->bhv", new_state, query_act, precision=lax.Precision.HIGHEST)
    readout = (
        readout
        * lax.rsqrt(jnp.mean(readout * readout, axis=2, keepdims=True) + epsilon)
        * head_gain
    )
    mixed_in = (
        readout.reshape(own_rows, local_heads * head_width) * jax.nn.silu(pre_gate_out)
    ).astype(jnp.bfloat16)
    partials = jnp.dot(
        lax.all_gather(mixed_in, "kv", axis=0, tiled=True),
        proj_out,
        preferred_element_type=jnp.float32,
    ).astype(jnp.bfloat16)
    mixed_sum = lax.psum_scatter(partials, "tp", scatter_dimension=1, tiled=True).astype(
        jnp.float32
    )
    second = (after_first.astype(jnp.float32) + mixed_sum).astype(jnp.bfloat16)
    hidden_two = half_inputs(second, post_gain, post_gate, post_up)
    result = (second.astype(jnp.float32) + 0.5 * down_sum(hidden_two, post_down)).astype(
        jnp.bfloat16
    )
    return (result, new_state)


LANES = 128
CORES = 2
F32, BF16 = jnp.float32, jnp.bfloat16
MESH = pl.DeviceIdType.MESH


class Grid:
    def __init__(self, n_kv, n_tp):
        self.nk, self.nt, self.nx = n_kv, n_tp, n_tp // CORES
        self.kv, self.tp = lax.axis_index("kv"), lax.axis_index("tp")
        self.x, self.c = self.tp // CORES, self.tp % CORES
        self.oc = 1 - self.c

    def k(self, step):
        return lax.rem(self.kv + step, self.nk)

    def xi(self, step):
        return lax.rem(self.x + step, self.nx)

    def t(self, step):
        return lax.rem(self.tp + step, self.nt)

    def block(self, k, x, c):
        return k * self.nt + x * CORES + c


def remote(src, dst, send, recv, k, t):
    return pltpu.make_async_remote_copy(
        src_ref=src, dst_ref=dst, send_sem=send, recv_sem=recv,
        device_id={"kv": k, "tp": t}, device_id_type=MESH,
    )


def barrier(g):
    sem = pltpu.get_barrier_semaphore()
    for step in range(1, g.nk):
        pl.semaphore_signal(sem, inc=1, device_id={"kv": g.k(step), "tp": g.tp}, device_id_type=MESH)
    for step in range(1, g.nt):
        pl.semaphore_signal(sem, inc=1, device_id={"kv": g.kv, "tp": g.t(step)}, device_id_type=MESH)
    pl.semaphore_wait(sem, g.nk - 1 + g.nt - 1)


def cols(ref, block, width=LANES):
    return ref.at[:, pl.ds(pl.multiple_of(block * width, LANES), width)]


def gather_all(g, own_ref, full, send_k, send_x, send_c, recv):
    started = []

    def put(src, block, sem, k, t):
        copy = remote(src, cols(full, block), sem, recv.at[block], k, t)
        copy.start()
        started.append(copy)

    def arrived(block):
        remote(own_ref, cols(full, block), send_k.at[0], recv.at[block], g.kv, g.tp).wait_recv()

    mine = g.block(g.kv, g.x, g.c)
    for step in range(1, g.nk):
        put(own_ref, mine, send_k.at[step], g.k(step), g.tp)
    for dx in range(1, g.nx):
        put(own_ref, mine, send_x.at[0, dx], g.kv, g.xi(dx) * CORES + g.c)
    put(own_ref, mine, send_c.at[0, 0], g.kv, g.x * CORES + g.oc)
    full[:, pl.ds(pl.multiple_of(mine * LANES, LANES), LANES)] = own_ref[...]

    def cross(step):
        k = g.k(g.nk - step)
        for dx in range(1, g.nx):
            block = g.block(k, g.xi(dx), g.c)
            arrived(block)
            put(cols(full, block), block, send_c.at[step, dx], g.kv, g.x * CORES + g.oc)

    for step in range(1, g.nk):
        block = g.block(g.k(g.nk - step), g.x, g.c)
        arrived(block)
        for dx in range(1, g.nx):
            put(cols(full, block), block, send_x.at[step, dx], g.kv, g.xi(dx) * CORES + g.c)
        put(cols(full, block), block, send_c.at[step, 0], g.kv, g.x * CORES + g.oc)
        cross(step - 1)
    cross(g.nk - 1)
    for step in range(g.nk):
        for dx in range(g.nx):
            arrived(g.block(g.k(g.nk - step), g.xi(dx), g.oc))
    for copy in started:
        copy.wait_send()


def hidden_units(full, gain_ref, wg, wu, acc_g, acc_u, hidden, width):
    rows, depth = full.shape
    acc_g[...] = jnp.zeros_like(acc_g)
    acc_u[...] = jnp.zeros_like(acc_u)

    def body(i, squares):
        at = pl.ds(pl.multiple_of(i * width, LANES), width)
        x = full[:, at].astype(F32)
        u = (x * gain_ref[:, at]).astype(BF16)
        acc_g[...] += jnp.dot(u, wg[at, :], preferred_element_type=F32)
        acc_u[...] += jnp.dot(u, wu[at, :], preferred_element_type=F32)
        return squares + jnp.sum(x * x, axis=1, keepdims=True)

    squares = lax.fori_loop(0, depth // width, body, jnp.zeros((rows, 1), F32))
    scale = lax.rsqrt(squares / depth + epsilon)
    hidden[...] = (jax.nn.silu(scale * acc_g[...]) * (scale * acc_u[...])).astype(BF16)


def down_scatter(g, hidden, wd, part, sib, out_x, in_x, keep, out_k, in_k, sa, ra, sb, rb, sc, rc):
    width = g.nt * LANES
    last = g.nk - 1

    def kof(i):
        return g.k(i + 1)

    def copy_a(i, xx):
        src = cols(part, g.block(kof(i), xx, g.oc))
        return remote(src, sib.at[i, xx], sa.at[i, xx], ra.at[i, xx], g.kv, g.x * CORES + g.oc)

    def copy_b(i, dx):
        return remote(out_x.at[i, dx - 1], in_x.at[i, dx - 1], sb.at[i, dx - 1], rb.at[i, dx - 1], g.kv, g.xi(dx) * CORES + g.c)

    def copy_c(i):
        return remote(out_k.at[i], in_k.at[i], sc.at[i], rc.at[i], kof(i), g.tp)

    def stage_a(i):
        at = pl.ds(pl.multiple_of(kof(i) * width, LANES), width)
        part[:, at] = jnp.dot(hidden[...], wd[:, at], preferred_element_type=F32).astype(BF16)
        for xx in range(g.nx):
            copy_a(i, xx).start()

    def pair_sum(i, xx):
        at = pl.ds(pl.multiple_of(g.block(kof(i), xx, g.c) * LANES, LANES), LANES)
        return part[:, at].astype(F32) + sib[i, xx].astype(F32)

    def stage_b(i):
        for xx in range(g.nx):
            copy_a(i, xx).wait_recv()
        for dx in range(1, g.nx):
            out_x[i, dx - 1] = pair_sum(i, g.xi(dx)).astype(BF16)
            copy_b(i, dx).start()
        keep[i % 2] = pair_sum(i, g.x)

    def stage_c(i):
        for dx in range(1, g.nx):
            copy_b(i, dx).wait_recv()
        total = keep[i % 2]
        for dx in range(1, g.nx):
            total = total + in_x[i, dx - 1].astype(F32)
        return total

    def send_c(i):
        out_k[i] = stage_c(i).astype(BF16)
        copy_c(i).start()

    stage_a(0)
    stage_a(1)
    stage_b(0)

    def body(i, carry):
        stage_a(i)
        send_c(i - 2)
        stage_b(i - 1)
        return carry

    lax.fori_loop(2, g.nk, body, 0)
    send_c(last - 1)
    stage_b(last)
    total = stage_c(last)
    for i in range(last):
        copy_c(i).wait_recv()
        total = total + in_k[i].astype(F32)
    for i in range(g.nk):
        for xx in range(g.nx):
            copy_a(i, xx).wait_send()
        for dx in range(1, g.nx):
            copy_b(i, dx).wait_send()
        if i < last:
            copy_c(i).wait_send()
    return total


def ff_scratch(nk, nt, rows, depth, units):
    nx = nt // CORES
    dma = pltpu.SemaphoreType.DMA
    weights = [
        pltpu.VMEM((depth, units), BF16),
        pltpu.VMEM((depth, units), BF16),
        pltpu.VMEM((units, depth), BF16),
        dma((3,)),
    ]
    gather = [
        pltpu.VMEM((rows, depth), BF16),
        dma((nk,)),
        dma((nk, nx)),
        dma((nk, nx)),
        dma((nk * nt,)),
    ]
    mid = [pltpu.VMEM((rows, units), F32), pltpu.VMEM((rows, units), F32), pltpu.VMEM((rows, units), BF16)]
    scatter = [
        pltpu.VMEM((rows, depth), BF16),
        pltpu.VMEM((nk, nx, rows, LANES), BF16),
        pltpu.VMEM((nk, nx - 1, rows, LANES), BF16),
        pltpu.VMEM((nk, nx - 1, rows, LANES), BF16),
        pltpu.VMEM((2, rows, LANES), F32),
        pltpu.VMEM((nk - 1, rows, LANES), BF16),
        pltpu.VMEM((nk - 1, rows, LANES), BF16),
        dma((nk, nx)),
        dma((nk, nx)),
        dma((nk, nx - 1)),
        dma((nk, nx - 1)),
        dma((nk - 1,)),
        dma((nk - 1,)),
    ]
    return weights + gather + mid + scatter


N_FF = 4 + 5 + 3 + 13


def load_weights(hbm, vmem, sem):
    copies = [pltpu.make_async_copy(a, b, sem.at[i]) for i, (a, b) in enumerate(zip(hbm, vmem))]
    for copy in copies:
        copy.start()
    return copies


def run_ff(g, own_ref, gain_ref, loads, ff):
    wg, wu, wd, _ = ff[:4]
    full, send_k, send_x, send_c, recv = ff[4:9]
    acc_g, acc_u, hidden = ff[9:12]
    gather_all(g, own_ref, full, send_k, send_x, send_c, recv)
    loads[0].wait()
    loads[1].wait()
    hidden_units(full, gain_ref, wg, wu, acc_g, acc_u, hidden, full.shape[1] // g.nk)
    loads[2].wait()
    total = down_scatter(g, hidden, wd, *ff[12:])
    return own_ref[...].astype(F32) + 0.5 * total


def first_kernel(nk, nt, tok, gain, mgain, wg_h, wu_h, wd_h, q_h, f_h, v_h, o_h, first, projected, *scratch):
    g = Grid(nk, nt)
    ff, rest = scratch[:N_FF], scratch[N_FF:]
    mixw, mix_sem, block, bsend, brecv, normed, proj, got, sq, sq_got, psend, precv, qsend, qrecv = rest
    loads = load_weights((wg_h, wu_h, wd_h), ff[:3], ff[3])
    mix_loads = load_weights((q_h, f_h, v_h, o_h), [mixw.at[i] for i in range(4)], mix_sem)
    barrier(g)
    first[...] = run_ff(g, tok, gain, loads, ff).astype(BF16)

    copies = []
    for step in range(1, nt):
        copy = remote(first, cols(block, g.tp), bsend.at[step - 1], brecv.at[step - 1], g.kv, g.t(step))
        copy.start()
        copies.append(copy)
    block[:, pl.ds(pl.multiple_of(g.tp * LANES, LANES), LANES)] = first[...]
    for step in range(1, nt):
        src = g.t(nt - step)
        remote(first, cols(block, src), bsend.at[step - 1], brecv.at[step - 1], g.kv, src).wait_recv()
    width = block.shape[1]
    x = block[...].astype(F32)
    normed[...] = (x * mgain[:, pl.ds(pl.multiple_of(g.kv * width, LANES), width)]).astype(BF16)
    sq[...] = jnp.broadcast_to(jnp.sum(x * x, axis=1, keepdims=True), sq.shape)
    own_rows, inner = projected.shape[0], projected.shape[1] // 4

    def rows_of(k):
        return pl.ds(pl.multiple_of(k * own_rows, own_rows), own_rows)

    def q_copy(step):
        return remote(sq.at[rows_of(g.k(step))], sq_got.at[step - 1], qsend.at[step - 1], qrecv.at[step - 1], g.k(step), g.tp)

    def p_copy(i, step):
        return remote(
            proj.at[i, rows_of(g.k(step))], got.at[i, step - 1], psend.at[i, step - 1], precv.at[i, step - 1], g.k(step), g.tp
        )

    for step in range(1, nk):
        q_copy(step).start()
    for i in range(4):
        mix_loads[i].wait()
        proj[i] = jnp.dot(normed[...], mixw[i], preferred_element_type=F32).astype(BF16)
        for step in range(1, nk):
            p_copy(i, step).start()
    squares = sq[rows_of(g.kv), :]
    for step in range(1, nk):
        q_copy(step).wait_recv()
        squares = squares + sq_got[step - 1]
    scale = lax.rsqrt(squares[:, :1] / mgain.shape[1] + epsilon)
    for i in range(4):
        total = proj[i, rows_of(g.kv), :].astype(F32)
        for step in range(1, nk):
            p_copy(i, step).wait_recv()
            total = total + got[i, step - 1].astype(F32)
        projected[:, i * inner : (i + 1) * inner] = total * scale
    for copy in copies:
        copy.wait_send()
    for step in range(1, nk):
        q_copy(step).wait_send()
        for i in range(4):
            p_copy(i, step).wait_send()


def second_kernel(nk, nt, y, first, gain, po_h, wg_h, wu_h, wd_h, result, *scratch):
    g = Grid(nk, nt)
    ff, rest = scratch[:N_FF], scratch[N_FF:]
    po, po_sem, yfull, ysend, yrecv, part, got, tsend, trecv, second = rest
    po_load = load_weights((po_h,), (po,), po_sem)
    loads = load_weights((wg_h, wu_h, wd_h), ff[:3], ff[3])
    barrier(g)
    own_rows = y.shape[0]

    def rows_of(k):
        return pl.ds(pl.multiple_of(k * own_rows, own_rows), own_rows)

    def y_copy(step, k, src):
        return remote(y, yfull.at[rows_of(src)], ysend.at[step - 1], yrecv.at[step - 1], k, g.tp)

    for step in range(1, nk):
        y_copy(step, g.k(step), g.kv).start()
    yfull[rows_of(g.kv), :] = y[...]
    for step in range(1, nk):
        y_copy(step, g.k(step), g.k(nk - step)).wait_recv()
    po_load[0].wait()
    part[...] = jnp.dot(yfull[...], po[...], preferred_element_type=F32).astype(BF16)

    def t_copy(step):
        return remote(cols(part, g.t(step)), got.at[step - 1], tsend.at[step - 1], trecv.at[step - 1], g.kv, g.t(step))

    for step in range(1, nt):
        t_copy(step).start()
    total = part[:, pl.ds(pl.multiple_of(g.tp * LANES, LANES), LANES)].astype(F32)
    for step in range(1, nt):
        t_copy(step).wait_recv()
        total = total + got[step - 1].astype(F32)
    second[...] = (first[...].astype(F32) + total).astype(BF16)
    result[...] = run_ff(g, second, gain, loads, ff).astype(BF16)
    for step in range(1, nk):
        y_copy(step, g.k(step), g.kv).wait_send()
    for step in range(1, nt):
        t_copy(step).wait_send()


def call(kernel, ident, outs, n_vmem, n_any, scratch, args):
    vmem, any_space = pl.BlockSpec(memory_space=pltpu.VMEM), pl.BlockSpec(memory_space=pl.ANY)
    return pl.pallas_call(
        kernel,
        out_shape=outs,
        in_specs=[vmem] * n_vmem + [any_space] * n_any,
        out_specs=jax.tree.map(lambda _: vmem, outs),
        scratch_shapes=scratch,
        compiler_params=pltpu.CompilerParams(
            collective_id=ident, has_side_effects=True, vmem_limit_bytes=56 * 1024 * 1024
        ),
    )(*args)


def per_device(
    tokens, past_state, pre_gain, pre_gate, pre_up, pre_down, mix_gain,
    query_weight, forget_weight, value_weight, output_gate_weight,
    forget_floor, head_gain, proj_out, post_gain, post_gate, post_up, post_down,
):
    nk, nt = lax.axis_size("kv"), lax.axis_size("tp")
    rows, depth, units = tokens.shape[0], pre_gate.shape[0], pre_gate.shape[1]
    own_rows, local_heads, head_width = past_state.shape[:3]
    inner = local_heads * head_width
    width = query_weight.shape[0]
    dma = pltpu.SemaphoreType.DMA
    base = ff_scratch(nk, nt, rows, depth, units)
    first, projected = call(
        functools.partial(first_kernel, nk, nt),
        0,
        (jax.ShapeDtypeStruct(tokens.shape, BF16), jax.ShapeDtypeStruct((own_rows, 4 * inner), F32)),
        3,
        7,
        base
        + [
            pltpu.VMEM((4, width, inner), BF16),
            dma((4,)),
            pltpu.VMEM((rows, width), BF16),
            dma((nt - 1,)),
            dma((nt - 1,)),
            pltpu.VMEM((rows, width), BF16),
            pltpu.VMEM((4, rows, inner), BF16),
            pltpu.VMEM((4, nk - 1, own_rows, inner), BF16),
            pltpu.VMEM((rows, LANES), F32),
            pltpu.VMEM((nk - 1, own_rows, LANES), F32),
            dma((4, nk - 1)),
            dma((4, nk - 1)),
            dma((nk - 1,)),
            dma((nk - 1,)),
        ],
        (
            tokens, pre_gain[None], mix_gain[None], pre_gate, pre_up, pre_down,
            query_weight, forget_weight, value_weight, output_gate_weight,
        ),
    )
    pre_query, pre_forget, pre_value, pre_gate_out = jnp.split(projected, 4, axis=1)
    head_shape = (own_rows, local_heads, head_width)
    floors = forget_floor.reshape(local_heads, head_width)
    forget_heads = pre_forget.reshape(head_shape)
    forget = floors + (1.0 - floors) * jax.nn.sigmoid(forget_heads)
    written = (1.0 - floors) * jax.nn.sigmoid(-forget_heads)
    query_act = jax.nn.silu(pre_query.reshape(head_shape))
    value_act = pre_value.reshape(head_shape)
    new_state = (
        forget[:, :, :, None] * past_state + written[:, :, :, None] * value_act[:, :, None, :]
    )
    readout = jnp.einsum("bhkv,bhk->bhv", new_state, query_act, precision=lax.Precision.HIGHEST)
    readout = (
        readout
        * lax.rsqrt(jnp.mean(readout * readout, axis=2, keepdims=True) + epsilon)
        * head_gain
    )
    mixed_in = (readout.reshape(own_rows, inner) * jax.nn.silu(pre_gate_out)).astype(BF16)
    result = call(
        functools.partial(second_kernel, nk, nt),
        1,
        jax.ShapeDtypeStruct(tokens.shape, BF16),
        3,
        4,
        base
        + [
            pltpu.VMEM(proj_out.shape, BF16),
            dma((1,)),
            pltpu.VMEM((rows, inner), BF16),
            dma((nk - 1,)),
            dma((nk - 1,)),
            pltpu.VMEM((rows, width), BF16),
            pltpu.VMEM((nt - 1, rows, LANES), BF16),
            dma((nt - 1,)),
            dma((nt - 1,)),
            pltpu.VMEM((rows, LANES), BF16),
        ],
        (mixed_in, first, post_gain[None], proj_out, post_gate, post_up, post_down),
    )
    return (result, new_state)


def solution(mesh):
    placed = (
        P(None, ("kv", "tp")),
        P("kv", "tp", None, None),
        P(),
        P(None, ("kv", "tp")),
        P(None, ("kv", "tp")),
        P(("kv", "tp"), None),
        P(),
        P("kv", "tp"),
        P("kv", "tp"),
        P("kv", "tp"),
        P("kv", "tp"),
        P("tp"),
        P(),
        P("tp", "kv"),
        P(),
        P(None, ("kv", "tp")),
        P(None, ("kv", "tp")),
        P(("kv", "tp"), None),
    )
    blocks_fit = D == mesh.shape["kv"] * mesh.shape["tp"] * LANES and mesh.shape["tp"] >= 2 * CORES
    return jax.shard_map(
        per_device if blocks_fit else per_device_plain,
        mesh=mesh,
        in_specs=placed,
        out_specs=(P(None, ("kv", "tp")), P("kv", "tp", None, None)),
        check_vma=False,
    )
```

```python
import functools

import jax
import jax.numpy as jnp
from jax import lax
from jax.experimental import pallas as pl
from jax.experimental.pallas import tpu as pltpu
from jax.sharding import PartitionSpec as P

D = 4096


epsilon = 1e-06


def half_inputs(activations, gain, w_gate, w_up):
    piece_float = lax.all_gather(activations, ("kv", "tp"), axis=1, tiled=True).astype(jnp.float32)
    normed = (piece_float * gain).astype(jnp.bfloat16)
    gate_acc = jnp.dot(normed, w_gate, preferred_element_type=jnp.float32)
    up_acc = jnp.dot(normed, w_up, preferred_element_type=jnp.float32)
    squares = jnp.sum(piece_float * piece_float, axis=1)
    row_scale = lax.rsqrt(squares / D + epsilon)[:, None]
    return (jax.nn.silu(row_scale * gate_acc) * (row_scale * up_acc)).astype(jnp.bfloat16)


def down_sum(hidden, w_down):
    return lax.psum_scatter(
        jnp.dot(hidden, w_down, preferred_element_type=jnp.float32),
        ("kv", "tp"),
        scatter_dimension=1,
        tiled=True,
    )


def per_device_plain(
    tokens,
    past_state,
    pre_gain,
    pre_gate,
    pre_up,
    pre_down,
    mix_gain,
    query_weight,
    forget_weight,
    value_weight,
    output_gate_weight,
    forget_floor,
    head_gain,
    proj_out,
    post_gain,
    post_gate,
    post_up,
    post_down,
):
    whole_rows = lax.all_gather(tokens, ("kv", "tp"), axis=1, tiled=True)
    whole_float = whole_rows.astype(jnp.float32)
    row_scale = lax.rsqrt(jnp.mean(whole_float * whole_float, axis=1, keepdims=True) + epsilon)
    normed = (whole_float * pre_gain).astype(jnp.bfloat16)
    gate_pre = row_scale * jnp.dot(normed, pre_gate, preferred_element_type=jnp.float32)
    up_pre = row_scale * jnp.dot(normed, pre_up, preferred_element_type=jnp.float32)
    hidden = (jax.nn.silu(gate_pre) * up_pre).astype(jnp.bfloat16)
    kv_sums = lax.psum_scatter(
        jnp.dot(hidden, pre_down, preferred_element_type=jnp.float32).astype(jnp.bfloat16),
        "kv",
        scatter_dimension=1,
        tiled=True,
    )
    block_sum = lax.psum(kv_sums, "tp").astype(jnp.float32)
    block_width = block_sum.shape[1]
    block_old = lax.dynamic_slice_in_dim(
        whole_rows, lax.axis_index("kv") * block_width, block_width, 1
    )
    block_rows = (block_old.astype(jnp.float32) + 0.5 * block_sum).astype(jnp.bfloat16)
    own_width = block_width // lax.axis_size("tp")
    after_first = lax.dynamic_slice_in_dim(
        block_rows, lax.axis_index("tp") * own_width, own_width, 1
    )
    block_width = block_rows.shape[1]
    block_float = block_rows.astype(jnp.float32)
    block_gain = lax.dynamic_slice_in_dim(
        mix_gain, lax.axis_index("kv") * block_width, block_width, 0
    )
    squares = lax.psum(jnp.sum(block_float * block_float, axis=1), "kv")
    normed = (block_float * block_gain).astype(jnp.bfloat16)
    own_rows = past_state.shape[0]
    weight_list = (query_weight, forget_weight, value_weight, output_gate_weight)
    projected = lax.psum_scatter(
        jnp.concatenate(
            [
                jnp.dot(normed, weight_part, preferred_element_type=jnp.float32)
                for weight_part in weight_list
            ],
            axis=1,
        ).astype(jnp.bfloat16),
        "kv",
        scatter_dimension=0,
        tiled=True,
    ).astype(jnp.float32)
    own_squares = lax.dynamic_slice_in_dim(squares, lax.axis_index("kv") * own_rows, own_rows, 0)
    projected = projected * lax.rsqrt(own_squares / D + epsilon)[:, None]
    pre_query, pre_forget, pre_value, pre_gate_out = jnp.split(projected, 4, axis=1)
    local_heads = past_state.shape[1]
    head_width = past_state.shape[2]
    head_shape = (own_rows, local_heads, head_width)
    floors = forget_floor.reshape(local_heads, head_width)
    forget_heads = pre_forget.reshape(head_shape)
    forget = floors + (1.0 - floors) * jax.nn.sigmoid(forget_heads)
    written = (1.0 - floors) * jax.nn.sigmoid(-forget_heads)
    query_act = jax.nn.silu(pre_query.reshape(head_shape))
    value_act = pre_value.reshape(head_shape)
    new_state = (
        forget[:, :, :, None] * past_state + written[:, :, :, None] * value_act[:, :, None, :]
    )
    readout = jnp.einsum("bhkv,bhk->bhv", new_state, query_act, precision=lax.Precision.HIGHEST)
    readout = (
        readout
        * lax.rsqrt(jnp.mean(readout * readout, axis=2, keepdims=True) + epsilon)
        * head_gain
    )
    mixed_in = (
        readout.reshape(own_rows, local_heads * head_width) * jax.nn.silu(pre_gate_out)
    ).astype(jnp.bfloat16)
    partials = jnp.dot(
        lax.all_gather(mixed_in, "kv", axis=0, tiled=True),
        proj_out,
        preferred_element_type=jnp.float32,
    ).astype(jnp.bfloat16)
    mixed_sum = lax.psum_scatter(partials, "tp", scatter_dimension=1, tiled=True).astype(
        jnp.float32
    )
    second = (after_first.astype(jnp.float32) + mixed_sum).astype(jnp.bfloat16)
    hidden_two = half_inputs(second, post_gain, post_gate, post_up)
    result = (second.astype(jnp.float32) + 0.5 * down_sum(hidden_two, post_down)).astype(
        jnp.bfloat16
    )
    return (result, new_state)


LANES = 128
LAST = (((1,), (1,)), ((), ()))
CORES = 2
F32, BF16 = jnp.float32, jnp.bfloat16
MESH = pl.DeviceIdType.MESH


class Grid:
    def __init__(self, n_kv, n_tp):
        self.nk, self.nt, self.nx = n_kv, n_tp, n_tp // CORES
        self.kv, self.tp = lax.axis_index("kv"), lax.axis_index("tp")
        self.x, self.c = self.tp // CORES, self.tp % CORES
        self.oc = 1 - self.c

    def k(self, step):
        return lax.rem(self.kv + step, self.nk)

    def xi(self, step):
        return lax.rem(self.x + step, self.nx)

    def t(self, step):
        return lax.rem(self.tp + step, self.nt)

    def block(self, k, x, c):
        return k * self.nt + x * CORES + c


def remote(src, dst, send, recv, k, t):
    return pltpu.make_async_remote_copy(
        src_ref=src, dst_ref=dst, send_sem=send, recv_sem=recv,
        device_id={"kv": k, "tp": t}, device_id_type=MESH,
    )


def barrier(g):
    sem = pltpu.get_barrier_semaphore()
    for step in range(1, g.nk):
        pl.semaphore_signal(sem, inc=1, device_id={"kv": g.k(step), "tp": g.tp}, device_id_type=MESH)
    for step in range(1, g.nt):
        pl.semaphore_signal(sem, inc=1, device_id={"kv": g.kv, "tp": g.t(step)}, device_id_type=MESH)
    pl.semaphore_wait(sem, g.nk - 1 + g.nt - 1)


def cols(ref, block, width=LANES):
    return ref.at[:, pl.ds(pl.multiple_of(block * width, LANES), width)]


def gather_all(g, own_ref, full, send_k, send_x, send_c, recv):
    started = []

    def put(src, block, sem, k, t):
        copy = remote(src, cols(full, block), sem, recv.at[block], k, t)
        copy.start()
        started.append(copy)

    def arrived(block):
        remote(own_ref, cols(full, block), send_k.at[0], recv.at[block], g.kv, g.tp).wait_recv()

    mine = g.block(g.kv, g.x, g.c)
    for step in range(1, g.nk):
        put(own_ref, mine, send_k.at[step], g.k(step), g.tp)
    for dx in range(1, g.nx):
        put(own_ref, mine, send_x.at[0, dx], g.kv, g.xi(dx) * CORES + g.c)
    put(own_ref, mine, send_c.at[0, 0], g.kv, g.x * CORES + g.oc)
    full[:, pl.ds(pl.multiple_of(mine * LANES, LANES), LANES)] = own_ref[...]

    def cross(step):
        k = g.k(g.nk - step)
        for dx in range(1, g.nx):
            block = g.block(k, g.xi(dx), g.c)
            arrived(block)
            put(cols(full, block), block, send_c.at[step, dx], g.kv, g.x * CORES + g.oc)

    for step in range(1, g.nk):
        block = g.block(g.k(g.nk - step), g.x, g.c)
        arrived(block)
        for dx in range(1, g.nx):
            put(cols(full, block), block, send_x.at[step, dx], g.kv, g.xi(dx) * CORES + g.c)
        put(cols(full, block), block, send_c.at[step, 0], g.kv, g.x * CORES + g.oc)
        cross(step - 1)
    cross(g.nk - 1)
    for step in range(g.nk):
        for dx in range(g.nx):
            arrived(g.block(g.k(g.nk - step), g.xi(dx), g.oc))
    for copy in started:
        copy.wait_send()


def hidden_units(full, gain_ref, wg, wu, acc_g, acc_u, hidden, width):
    rows, depth = full.shape
    acc_g[...] = jnp.zeros_like(acc_g)
    acc_u[...] = jnp.zeros_like(acc_u)

    def body(i, squares):
        at = pl.ds(pl.multiple_of(i * width, LANES), width)
        x = full[:, at].astype(F32)
        u = (x * gain_ref[:, at]).astype(BF16)
        acc_g[...] += lax.dot_general(u, wg[:, at], LAST, preferred_element_type=F32)
        acc_u[...] += lax.dot_general(u, wu[:, at], LAST, preferred_element_type=F32)
        return squares + jnp.sum(x * x, axis=1, keepdims=True)

    squares = lax.fori_loop(0, depth // width, body, jnp.zeros((rows, 1), F32))
    scale = lax.rsqrt(squares / depth + epsilon)
    hidden[...] = (jax.nn.silu(scale * acc_g[...]) * (scale * acc_u[...])).astype(BF16)


def down_scatter(g, hidden, wd, part, sib, out_x, in_x, keep, out_k, in_k, sa, ra, sb, rb, sc, rc):
    width = g.nt * LANES
    last = g.nk - 1

    def kof(i):
        return g.k(i + 1)

    def copy_a(i, xx):
        src = cols(part, g.block(kof(i), xx, g.oc))
        return remote(src, sib.at[i, xx], sa.at[i, xx], ra.at[i, xx], g.kv, g.x * CORES + g.oc)

    def copy_b(i, dx):
        return remote(out_x.at[i, dx - 1], in_x.at[i, dx - 1], sb.at[i, dx - 1], rb.at[i, dx - 1], g.kv, g.xi(dx) * CORES + g.c)

    def copy_c(i):
        return remote(out_k.at[i], in_k.at[i], sc.at[i], rc.at[i], kof(i), g.tp)

    def stage_a(i):
        at = pl.ds(pl.multiple_of(kof(i) * width, LANES), width)
        part[:, at] = jnp.dot(hidden[...], wd[:, at], preferred_element_type=F32).astype(BF16)
        for xx in range(g.nx):
            copy_a(i, xx).start()

    def pair_sum(i, xx):
        at = pl.ds(pl.multiple_of(g.block(kof(i), xx, g.c) * LANES, LANES), LANES)
        return part[:, at].astype(F32) + sib[i, xx].astype(F32)

    def stage_b(i):
        for xx in range(g.nx):
            copy_a(i, xx).wait_recv()
        for dx in range(1, g.nx):
            out_x[i, dx - 1] = pair_sum(i, g.xi(dx)).astype(BF16)
            copy_b(i, dx).start()
        keep[i % 2] = pair_sum(i, g.x)

    def stage_c(i):
        for dx in range(1, g.nx):
            copy_b(i, dx).wait_recv()
        total = keep[i % 2]
        for dx in range(1, g.nx):
            total = total + in_x[i, dx - 1].astype(F32)
        return total

    def send_c(i):
        out_k[i] = stage_c(i).astype(BF16)
        copy_c(i).start()

    stage_a(0)
    stage_a(1)
    stage_b(0)

    def body(i, carry):
        stage_a(i)
        send_c(i - 2)
        stage_b(i - 1)
        return carry

    lax.fori_loop(2, g.nk, body, 0)
    send_c(last - 1)
    stage_b(last)
    total = stage_c(last)
    for i in range(last):
        copy_c(i).wait_recv()
        total = total + in_k[i].astype(F32)
    for i in range(g.nk):
        for xx in range(g.nx):
            copy_a(i, xx).wait_send()
        for dx in range(1, g.nx):
            copy_b(i, dx).wait_send()
        if i < last:
            copy_c(i).wait_send()
    return total


def ff_scratch(nk, nt, rows, depth, units):
    nx = nt // CORES
    dma = pltpu.SemaphoreType.DMA
    weights = [
        pltpu.VMEM((units, depth), BF16),
        pltpu.VMEM((units, depth), BF16),
        pltpu.VMEM((units, depth), BF16),
        dma((3,)),
    ]
    gather = [
        pltpu.VMEM((rows, depth), BF16),
        dma((nk,)),
        dma((nk, nx)),
        dma((nk, nx)),
        dma((nk * nt,)),
    ]
    mid = [pltpu.VMEM((rows, units), F32), pltpu.VMEM((rows, units), F32), pltpu.VMEM((rows, units), BF16)]
    scatter = [
        pltpu.VMEM((rows, depth), BF16),
        pltpu.VMEM((nk, nx, rows, LANES), BF16),
        pltpu.VMEM((nk, nx - 1, rows, LANES), BF16),
        pltpu.VMEM((nk, nx - 1, rows, LANES), BF16),
        pltpu.VMEM((2, rows, LANES), F32),
        pltpu.VMEM((nk - 1, rows, LANES), BF16),
        pltpu.VMEM((nk - 1, rows, LANES), BF16),
        dma((nk, nx)),
        dma((nk, nx)),
        dma((nk, nx - 1)),
        dma((nk, nx - 1)),
        dma((nk - 1,)),
        dma((nk - 1,)),
    ]
    return weights + gather + mid + scatter


N_FF = 4 + 5 + 3 + 13


def load_weights(hbm, vmem, sem):
    copies = [pltpu.make_async_copy(a, b, sem.at[i]) for i, (a, b) in enumerate(zip(hbm, vmem))]
    for copy in copies:
        copy.start()
    return copies


def run_ff(g, own_ref, gain_ref, loads, ff):
    wg, wu, wd, _ = ff[:4]
    full, send_k, send_x, send_c, recv = ff[4:9]
    acc_g, acc_u, hidden = ff[9:12]
    gather_all(g, own_ref, full, send_k, send_x, send_c, recv)
    loads[0].wait()
    loads[1].wait()
    hidden_units(full, gain_ref, wg, wu, acc_g, acc_u, hidden, full.shape[1] // g.nk)
    loads[2].wait()
    total = down_scatter(g, hidden, wd, *ff[12:])
    return own_ref[...].astype(F32) + 0.5 * total


def first_kernel(nk, nt, tok, gain, mgain, wg_h, wu_h, wd_h, q_h, f_h, v_h, o_h, first, projected, *scratch):
    g = Grid(nk, nt)
    ff, rest = scratch[:N_FF], scratch[N_FF:]
    mixw, mix_sem, block, bsend, brecv, normed, proj, mate_got, sums, got, sq, sq_got, msend, mrecv, psend, precv, qsend, qrecv = rest
    loads = load_weights((wg_h, wu_h, wd_h), ff[:3], ff[3])
    mix_loads = load_weights((q_h, f_h, v_h, o_h), [mixw.at[i] for i in range(4)], mix_sem)
    barrier(g)
    first[...] = run_ff(g, tok, gain, loads, ff).astype(BF16)

    copies = []
    for step in range(1, nt):
        copy = remote(first, cols(block, g.tp), bsend.at[step - 1], brecv.at[step - 1], g.kv, g.t(step))
        copy.start()
        copies.append(copy)
    block[:, pl.ds(pl.multiple_of(g.tp * LANES, LANES), LANES)] = first[...]
    for step in range(1, nt):
        src = g.t(nt - step)
        remote(first, cols(block, src), bsend.at[step - 1], brecv.at[step - 1], g.kv, src).wait_recv()
    width = block.shape[1]
    x = block[...].astype(F32)
    normed[...] = (x * mgain[:, pl.ds(pl.multiple_of(g.kv * width, LANES), width)]).astype(BF16)
    sq[...] = jnp.broadcast_to(jnp.sum(x * x, axis=1, keepdims=True), sq.shape)
    own_rows, inner = projected.shape[0], projected.shape[1] // 4

    def rows_of(k):
        return pl.ds(pl.multiple_of(k * own_rows, own_rows), own_rows)

    def q_copy(step):
        return remote(sq.at[rows_of(g.k(step))], sq_got.at[step - 1], qsend.at[step - 1], qrecv.at[step - 1], g.k(step), g.tp)

    nz, z, y = nk // 2, g.kv // 2, g.kv % 2

    def zi(dz):
        return lax.rem(z + dz, nz)

    def m_copy(i, dz):
        src = proj.at[i, zi(dz) * 2 + 1 - y]
        return remote(src, mate_got.at[i, dz], msend.at[i, dz], mrecv.at[i, dz], 2 * z + 1 - y, g.tp)

    def p_copy(i, dz):
        at = dz - 1
        return remote(sums.at[i, at], got.at[i, at], psend.at[i, at], precv.at[i, at], zi(dz) * 2 + y, g.tp)

    def mate_sum(i, dz):
        m_copy(i, dz).wait_recv()
        return proj[i, zi(dz) * 2 + y].astype(F32) + mate_got[i, dz].astype(F32)

    def forward(i):
        for dz in range(1, nz):
            sums[i, dz - 1] = mate_sum(i, dz).astype(BF16)
            p_copy(i, dz).start()

    for step in range(1, nk):
        q_copy(step).start()
    for i in range(4):
        mix_loads[i].wait()
        out = jnp.dot(normed[...], mixw[i], preferred_element_type=F32).astype(BF16)
        proj[i] = out.reshape(nk, own_rows, inner)
        for dz in range(1, nz + 1):
            m_copy(i, dz % nz).start()
        if i:
            forward(i - 1)
    forward(3)
    squares = sq[rows_of(g.kv), :]
    for step in range(1, nk):
        q_copy(step).wait_recv()
        squares = squares + sq_got[step - 1]
    scale = lax.rsqrt(squares[:, :1] / mgain.shape[1] + epsilon)
    for i in range(4):
        total = mate_sum(i, 0)
        for dz in range(1, nz):
            p_copy(i, dz).wait_recv()
            total = total + got[i, dz - 1].astype(F32)
        projected[:, i * inner : (i + 1) * inner] = total * scale
    for copy in copies:
        copy.wait_send()
    for step in range(1, nk):
        q_copy(step).wait_send()
    for i in range(4):
        for dz in range(nz):
            m_copy(i, dz).wait_send()
        for dz in range(1, nz):
            p_copy(i, dz).wait_send()


def recurrence_kernel(projected, past, floor, head_gain, new, mixed):
    rows, heads, width = past.shape[:3]
    inner = heads * width
    for h in range(heads):
        def part(i):
            return projected[:, i * inner + h * width : i * inner + (h + 1) * width]

        at = slice(h * width, (h + 1) * width)
        base = floor[:, at]
        forget = (base + (1.0 - base) * jax.nn.sigmoid(part(1))).T
        written = ((1.0 - base) * jax.nn.sigmoid(-part(1))).T
        query = jax.nn.silu(part(0)).T
        value = part(2)
        outs = []
        for n in range(rows):
            col = slice(n, n + 1)
            state = forget[:, col] * past[n, h] + written[:, col] * value[col]
            new[n, h] = state
            outs.append(jnp.sum(state * query[:, col], axis=0, keepdims=True))
        read = jnp.concatenate(outs, axis=0)
        read = read * lax.rsqrt(jnp.mean(read * read, axis=1, keepdims=True) + epsilon) * head_gain[...]
        mixed[:, at] = (read * jax.nn.silu(part(3))).astype(BF16)


def recurrence(projected, past_state, forget_floor, head_gain):
    rows, heads, width = past_state.shape[:3]
    inner, step = heads * width, 8
    state_spec = pl.BlockSpec((step, heads, width, width), lambda i: (i, 0, 0, 0))
    return pl.pallas_call(
        recurrence_kernel,
        grid=(rows // step,),
        out_shape=(
            jax.ShapeDtypeStruct(past_state.shape, F32),
            jax.ShapeDtypeStruct((rows, inner), BF16),
        ),
        in_specs=[
            pl.BlockSpec((step, 4 * inner), lambda i: (i, 0)),
            state_spec,
            pl.BlockSpec((1, inner), lambda i: (0, 0)),
            pl.BlockSpec((1, width), lambda i: (0, 0)),
        ],
        out_specs=(state_spec, pl.BlockSpec((step, inner), lambda i: (i, 0))),
        compiler_params=pltpu.CompilerParams(vmem_limit_bytes=32 * 1024 * 1024),
    )(projected, past_state, forget_floor[None], head_gain[None])


def second_kernel(nk, nt, y, first, gain, po_h, wg_h, wu_h, wd_h, result, *scratch):
    g = Grid(nk, nt)
    ff, rest = scratch[:N_FF], scratch[N_FF:]
    po, po_sem, yfull, ysend, yrecv, part, got, tsend, trecv, second = rest
    po_load = load_weights((po_h,), (po,), po_sem)
    loads = load_weights((wg_h, wu_h, wd_h), ff[:3], ff[3])
    barrier(g)
    own_rows = y.shape[0]

    def rows_of(k):
        return pl.ds(pl.multiple_of(k * own_rows, own_rows), own_rows)

    def y_copy(step, k, src):
        return remote(y, yfull.at[rows_of(src)], ysend.at[step - 1], yrecv.at[step - 1], k, g.tp)

    for step in range(1, nk):
        y_copy(step, g.k(step), g.kv).start()
    yfull[rows_of(g.kv), :] = y[...]
    for step in range(1, nk):
        y_copy(step, g.k(step), g.k(nk - step)).wait_recv()
    po_load[0].wait()
    part[...] = jnp.dot(yfull[...], po[...], preferred_element_type=F32).astype(BF16)

    def t_copy(step):
        return remote(cols(part, g.t(step)), got.at[step - 1], tsend.at[step - 1], trecv.at[step - 1], g.kv, g.t(step))

    for step in range(1, nt):
        t_copy(step).start()
    total = part[:, pl.ds(pl.multiple_of(g.tp * LANES, LANES), LANES)].astype(F32)
    for step in range(1, nt):
        t_copy(step).wait_recv()
        total = total + got[step - 1].astype(F32)
    second[...] = (first[...].astype(F32) + total).astype(BF16)
    result[...] = run_ff(g, second, gain, loads, ff).astype(BF16)
    for step in range(1, nk):
        y_copy(step, g.k(step), g.kv).wait_send()
    for step in range(1, nt):
        t_copy(step).wait_send()


def call(kernel, ident, outs, n_vmem, n_any, scratch, args):
    vmem, any_space = pl.BlockSpec(memory_space=pltpu.VMEM), pl.BlockSpec(memory_space=pl.ANY)
    return pl.pallas_call(
        kernel,
        out_shape=outs,
        in_specs=[vmem] * n_vmem + [any_space] * n_any,
        out_specs=jax.tree.map(lambda _: vmem, outs),
        scratch_shapes=scratch,
        compiler_params=pltpu.CompilerParams(
            collective_id=ident, has_side_effects=True, vmem_limit_bytes=56 * 1024 * 1024
        ),
    )(*args)


def per_device(
    tokens, past_state, pre_gain, pre_gate, pre_up, pre_down, mix_gain,
    query_weight, forget_weight, value_weight, output_gate_weight,
    forget_floor, head_gain, proj_out, post_gain, post_gate, post_up, post_down,
):
    nk, nt = lax.axis_size("kv"), lax.axis_size("tp")
    rows, depth, units = tokens.shape[0], pre_gate.shape[0], pre_gate.shape[1]
    own_rows, local_heads, head_width = past_state.shape[:3]
    inner = local_heads * head_width
    width = query_weight.shape[0]
    dma = pltpu.SemaphoreType.DMA
    base = ff_scratch(nk, nt, rows, depth, units)
    first, projected = call(
        functools.partial(first_kernel, nk, nt),
        0,
        (jax.ShapeDtypeStruct(tokens.shape, BF16), jax.ShapeDtypeStruct((own_rows, 4 * inner), F32)),
        3,
        7,
        base
        + [
            pltpu.VMEM((4, width, inner), BF16),
            dma((4,)),
            pltpu.VMEM((rows, width), BF16),
            dma((nt - 1,)),
            dma((nt - 1,)),
            pltpu.VMEM((rows, width), BF16),
            pltpu.VMEM((4, nk, own_rows, inner), BF16),
            pltpu.VMEM((4, nk // 2, own_rows, inner), BF16),
            pltpu.VMEM((4, nk // 2 - 1, own_rows, inner), BF16),
            pltpu.VMEM((4, nk // 2 - 1, own_rows, inner), BF16),
            pltpu.VMEM((rows, LANES), F32),
            pltpu.VMEM((nk - 1, own_rows, LANES), F32),
            dma((4, nk // 2)),
            dma((4, nk // 2)),
            dma((4, nk // 2 - 1)),
            dma((4, nk // 2 - 1)),
            dma((nk - 1,)),
            dma((nk - 1,)),
        ],
        (
            tokens, pre_gain[None], mix_gain[None], pre_gate.T, pre_up.T, pre_down,
            query_weight, forget_weight, value_weight, output_gate_weight,
        ),
    )
    new_state, mixed_in = recurrence(projected, past_state, forget_floor, head_gain)
    result = call(
        functools.partial(second_kernel, nk, nt),
        1,
        jax.ShapeDtypeStruct(tokens.shape, BF16),
        3,
        4,
        base
        + [
            pltpu.VMEM(proj_out.shape, BF16),
            dma((1,)),
            pltpu.VMEM((rows, inner), BF16),
            dma((nk - 1,)),
            dma((nk - 1,)),
            pltpu.VMEM((rows, width), BF16),
            pltpu.VMEM((nt - 1, rows, LANES), BF16),
            dma((nt - 1,)),
            dma((nt - 1,)),
            pltpu.VMEM((rows, LANES), BF16),
        ],
        (mixed_in, first, post_gain[None], proj_out, post_gate.T, post_up.T, post_down),
    )
    return (result, new_state)


def solution(mesh):
    placed = (
        P(None, ("kv", "tp")),
        P("kv", "tp", None, None),
        P(),
        P(None, ("kv", "tp")),
        P(None, ("kv", "tp")),
        P(("kv", "tp"), None),
        P(),
        P("kv", "tp"),
        P("kv", "tp"),
        P("kv", "tp"),
        P("kv", "tp"),
        P("tp"),
        P(),
        P("tp", "kv"),
        P(),
        P(None, ("kv", "tp")),
        P(None, ("kv", "tp")),
        P(("kv", "tp"), None),
    )
    blocks_fit = D == mesh.shape["kv"] * mesh.shape["tp"] * LANES and mesh.shape["tp"] >= 2 * CORES
    return jax.shard_map(
        per_device if blocks_fit else per_device_plain,
        mesh=mesh,
        in_specs=placed,
        out_specs=(P(None, ("kv", "tp")), P("kv", "tp", None, None)),
        check_vma=False,
    )
```
